32 devices in a mesh: sp: 8 (over z, y), tp: 4 (over x, core).
Axes of the slice: x: 2, y: 2, z: 4, core: 2. Of those that a mesh axis runs over, the one named last changes fastest.
Arguments:
- stream: bfloat16 [2048, 2048], P('sp'), may hold values from -6 to 6
- attn_gain: float32 [2, 2048], replicated, may hold values from 0.1 to 1.9
- w_query: bfloat16 [2, 2048, 2048], P(None, None, 'tp'), may hold values from -0.125 to 0.125
- w_key: bfloat16 [2, 2048, 512], P(None, None, 'tp'), may hold values from -0.125 to 0.125
- w_value: bfloat16 [2, 2048, 512], P(None, None, 'tp'), may hold values from -0.125 to 0.125
- w_out: bfloat16 [2, 2048, 2048], P(None, 'tp'), may hold values from -1 to 1
- query_gain: float32 [2, 64], replicated, may hold values from 0.1 to 1.9
- key_gain: float32 [2, 64], replicated, may hold values from 0.1 to 1.9
- rel_bias: float32 [2, 32, 257], P(None, 'tp'), may hold values from -6 to 300
Outputs:
- result: bfloat16 [2048, 2048], P('sp', 'tp')
The draws below stay inside these ranges and needn't reach their ends.
All inputs are finite; a program needn't handle non-finite values.
Results may differ from the reference program's by a relative error of at most 0.02.
Values may be sent and summed in bfloat16 or wider, within the bound.
A program may use at most 64 MiB of HBM per device.

```python
import jax
import jax.numpy as jnp
from jax import lax

D = 2048
HEAD_DIM = 64
HEADS = 32
KV_HEADS = 8
SEG = 64
LEFT = 4
CLIP = 128
LAYERS = 2
TOKENS = 2048
N_TP = 4


def draw_rel_bias(key, part):
    subkeys = jax.random.split(jax.random.fold_in(key, 17), 1)
    shape = (LAYERS, HEADS, 2 * CLIP + 1)
    bias_table = jnp.clip(jax.random.normal(subkeys[0], shape, jnp.float32), -6.0, 6.0)
    return bias_table


def shard_levels(key, extent, cuts, least, high):
    level = 1.0
    for dim, parts in cuts:
        steps = jax.random.uniform(jax.random.fold_in(jax.random.fold_in(key, 6), dim), (parts,), jnp.float32, least / len(cuts), high / len(cuts))
        level = level * jnp.repeat(jnp.exp(steps), extent[dim] // parts).reshape((-1,) + (1,) * (len(extent) - 1 - dim))
    return level


def scatter_about(stream_key, extent, scale, bound, cuts=(), held_as=jnp.bfloat16):
    result = jax.random.normal(stream_key, extent, jnp.float32) * scale
    if len(cuts) > 0:
        result = shard_levels(stream_key, extent, cuts, -0.22, 0.18) * result
    return jnp.clip(result, min=-bound, max=bound).astype(held_as)


def setup_inputs(seed: int = 0) -> dict:
    arg_keys = jax.random.split(jax.random.key(seed), 10)
    return {
        "stream": scatter_about(arg_keys[0], (TOKENS, D), 1.0, 6.0, ((0, 8),)),
        "attn_gain": jnp.clip(1.0 + 0.18 * jax.random.normal(arg_keys[1], (LAYERS, D), jnp.float32), 0.1, 1.9),
        "w_query": scatter_about(arg_keys[2], (LAYERS, D, D), D ** -0.5, 0.125, ((2, 4),)),
        "w_key": scatter_about(arg_keys[3], (LAYERS, D, KV_HEADS * HEAD_DIM), D ** -0.5, 0.125, ((2, 4),)),
        "w_value": scatter_about(arg_keys[4], (LAYERS, D, KV_HEADS * HEAD_DIM), D ** -0.5, 0.125, ((2, 4),)),
        "w_out": scatter_about(arg_keys[5], (LAYERS, D, D), (D // 64) ** -0.5, 1.0, ((1, 4),)),
        "query_gain": jnp.clip(1.0 + 0.18 * jax.random.normal(arg_keys[6], (LAYERS, HEAD_DIM), jnp.float32), 0.1, 1.9),
        "key_gain": jnp.clip(1.0 + 0.18 * jax.random.normal(arg_keys[7], (LAYERS, HEAD_DIM), jnp.float32), 0.1, 1.9),
        "rel_bias": draw_rel_bias(jax.random.fold_in(arg_keys[9], 71), 0),
    }


norm_eps = 1e-06
masked_score = -1e+30

def rms_scale(values_in, gain):
    squared = lax.optimization_barrier(jnp.mean(values_in * values_in, axis=-1, keepdims=True))
    return values_in * lax.rsqrt(squared + norm_eps) * gain

def bias_block(bias_table, key_reach):
    query_pos = jnp.arange(key_reach, dtype=jnp.int32)[:, None]
    key_pos = jnp.arange(2 * key_reach, dtype=jnp.int32)[None, :]
    distance = jnp.clip(query_pos + key_reach - key_pos, -CLIP, CLIP) + CLIP
    return bias_table[:, distance].astype(jnp.float32)

def band_mask(key_reach, first_query):
    query_pos = jnp.arange(key_reach, dtype=jnp.int32)[:, None]
    key_pos = jnp.arange(2 * key_reach, dtype=jnp.int32)[None, :] - key_reach
    query_seg = query_pos // SEG
    key_seg = key_pos // SEG
    return (key_seg <= query_seg) & (key_seg >= query_seg - LEFT) & (first_query + key_pos >= 0)

def band_attention(queries, keys_all, values_all, bias_table):
    key_reach = LEFT * SEG
    group = HEADS // KV_HEADS
    total_rows = queries.shape[0]
    bias = bias_block(bias_table, key_reach).reshape(KV_HEADS, group, key_reach, 2 * key_reach)

    def one_block(block_index):
        start = block_index * key_reach
        query_rows = lax.dynamic_slice_in_dim(queries, start, key_reach, 0).reshape(key_reach, KV_HEADS, group, HEAD_DIM)
        key_rows = lax.dynamic_slice_in_dim(keys_all, start, 2 * key_reach, 0)
        value_rows = lax.dynamic_slice_in_dim(values_all, start, 2 * key_reach, 0)
        scores = jnp.einsum('qkgd,jkd->kgqj', query_rows.astype(jnp.float32), key_rows.astype(jnp.float32)) * HEAD_DIM ** (-0.5) + bias
        inside = band_mask(key_reach, start)
        scores = jnp.where(inside, scores, masked_score)
        peak = lax.optimization_barrier(jnp.max(scores, axis=-1, keepdims=True))
        expon = jnp.exp(scores - peak)
        weights = lax.optimization_barrier((expon / lax.optimization_barrier(jnp.sum(expon, axis=-1, keepdims=True))).astype(jnp.bfloat16))
        mixed = jnp.einsum('kgqj,jkd->qkgd', weights.astype(jnp.float32), value_rows.astype(jnp.float32))
        return mixed.astype(jnp.bfloat16).reshape(key_reach, HEADS * HEAD_DIM)
    blocks = lax.map(one_block, jnp.arange(total_rows // key_reach, dtype=jnp.int32))
    return blocks.reshape(total_rows, HEADS * HEAD_DIM)

def reference(stream, attn_gain, w_query, w_key, w_value, w_out, query_gain, key_gain, rel_bias):
    current = stream
    total_rows = stream.shape[0]
    key_reach = LEFT * SEG
    head_cols = D // N_TP
    for layer_index in range(LAYERS):
        normed = rms_scale(current.astype(jnp.float32), attn_gain[layer_index]).astype(jnp.bfloat16)
        query_flat = jnp.dot(normed, w_query[layer_index], preferred_element_type=jnp.float32)
        queries = rms_scale(query_flat.reshape(total_rows, HEADS, HEAD_DIM), query_gain[layer_index]).astype(jnp.bfloat16)
        key_flat = jnp.dot(normed, w_key[layer_index], preferred_element_type=jnp.float32)
        keys_now = rms_scale(key_flat.reshape(total_rows, KV_HEADS, HEAD_DIM), key_gain[layer_index]).astype(jnp.bfloat16)
        values_now = jnp.dot(normed, w_value[layer_index], preferred_element_type=jnp.float32).astype(jnp.bfloat16).reshape(total_rows, KV_HEADS, HEAD_DIM)
        padding = jnp.zeros((key_reach, KV_HEADS, HEAD_DIM), jnp.bfloat16)
        keys_all = jnp.concatenate([padding, keys_now], axis=0)
        values_all = jnp.concatenate([padding, values_now], axis=0)
        mixed = band_attention(queries, keys_all, values_all, rel_bias[layer_index])
        update = jnp.zeros((total_rows, D), jnp.float32)
        for group_index in range(N_TP):
            lower = group_index * head_cols
            partial_value = jnp.dot(mixed[:, lower:lower + head_cols], w_out[layer_index, lower:lower + head_cols], preferred_element_type=jnp.float32)
            update = update + lax.optimization_barrier(partial_value.astype(jnp.bfloat16)).astype(jnp.float32)
        current = (current.astype(jnp.float32) + update).astype(jnp.bfloat16)
    return current
```

```python
import functools

import jax
import jax.numpy as jnp
from jax import lax
from jax.experimental import pallas as pl
from jax.experimental.pallas import tpu as pltpu
from jax.sharding import PartitionSpec as P

HEAD_DIM = 64
SEG = 64
LEFT = 4
CLIP = 128
LAYERS = 2
SPAN = (LEFT + 1) * SEG
LINE = 384

norm_eps = 1e-06
masked_score = -1e30
F32 = jnp.float32
BF16 = jnp.bfloat16


def seg_rows(seg):
    return pl.ds(pl.multiple_of(seg * SEG, SEG), SEG)


def send(src, dst, send_sem, recv_sem, device):
    return pltpu.make_async_remote_copy(
        src_ref=src,
        dst_ref=dst,
        send_sem=send_sem,
        recv_sem=recv_sem,
        device_id=device,
        device_id_type=pl.DeviceIdType.MESH,
    )


def row_norm(x, gain):
    squared = jnp.mean(x * x, axis=-1, keepdims=True)
    return (x * lax.rsqrt(squared + norm_eps) * gain).astype(BF16)


def head_norm(x, gain_row, scale):
    width = x.shape[1]
    block = min(width, 256)
    row_head = lax.broadcasted_iota(jnp.int32, (block, block), 0) >> 6
    col_head = lax.broadcasted_iota(jnp.int32, (block, block), 1) >> 6
    spread = jnp.where(row_head == col_head, 1.0 / HEAD_DIM, 0.0).astype(BF16)
    gain = jnp.concatenate([gain_row] * (block // HEAD_DIM), axis=1) * scale
    outs = []
    for lower in range(0, width, block):
        part = x[:, lower : lower + block]
        squares = part * part
        high = squares.astype(BF16)
        low = (squares - high.astype(F32)).astype(BF16)
        mean = jnp.dot(high, spread, preferred_element_type=F32) + jnp.dot(
            low, spread, preferred_element_type=F32
        )
        outs.append((part * lax.rsqrt(mean + norm_eps) * gain).astype(BF16))
    return outs[0] if len(outs) == 1 else jnp.concatenate(outs, axis=1)


def body(
    n_sp, n_tp,
    stream, attn_gain, w_query, w_key, w_value, w_out, query_gain, key_gain, rel_bias,
    out,
    cur0, cur1, normed, wq, wk, wv, wo, queries, pair_made, halo, kdup, vdup, bias, mixed,
    psend, precv, own0, xsend, xrecv,
    psend1, precv1, own1, xsend1, xrecv1,
    w_sem, ps_sem, pr_sem, xs_sem, xr_sem, cs_sem, cr_sem, hs_sem, hr_sem,
    ps1_sem, pr1_sem, xs1_sem, xr1_sem,
):
    row_count, width = cur0.shape
    segs = row_count // SEG
    half = segs // 2
    q_width = wq.shape[2]
    kv_width = wk.shape[2]
    heads = q_width // HEAD_DIM
    kv_heads = kv_width // HEAD_DIM
    group = heads // kv_heads
    n_x = n_tp // 2
    feat = width // n_tp
    me_sp = lax.axis_index("sp")
    me_tp = lax.axis_index("tp")
    core = lax.rem(me_tp, 2)
    chip = lax.div(me_tp, 2)
    partner = {"tp": chip * 2 + 1 - core}

    def chip_at(k):
        return lax.rem(chip + k, n_x)

    def peer(k):
        return {"tp": chip_at(k) * 2 + core}

    loads = []

    def load(src, dst):
        copy = pltpu.make_async_copy(src, dst, w_sem.at[len(loads)])
        copy.start()
        loads.append(copy)
        return copy

    stream_load = load(stream, cur0)
    weight_loads = []
    for l in range(LAYERS):
        weight_loads.append(
            [
                load(w_key.at[l], wk.at[l]),
                load(w_value.at[l], wv.at[l]),
                load(w_query.at[l], wq.at[l]),
                load(w_out.at[l], wo.at[l]),
            ]
        )

    barrier = pltpu.get_barrier_semaphore()
    pl.semaphore_signal(barrier, inc=1, device_id=partner, device_id_type=pl.DeviceIdType.MESH)
    for k in range(1, n_x):
        pl.semaphore_signal(barrier, inc=1, device_id=peer(k), device_id_type=pl.DeviceIdType.MESH)

    @pl.when(me_sp > 0)
    def _():
        pl.semaphore_signal(
            barrier, inc=1, device_id={"sp": me_sp - 1}, device_id_type=pl.DeviceIdType.MESH
        )

    @pl.when(me_sp < n_sp - 1)
    def _():
        pl.semaphore_signal(
            barrier, inc=1, device_id={"sp": me_sp + 1}, device_id_type=pl.DeviceIdType.MESH
        )

    offset = lax.broadcasted_iota(jnp.int32, (2 * CLIP, LINE), 1)
    distance = jnp.clip(LEFT * SEG + SEG - 1 - offset, -CLIP, CLIP) + CLIP
    onehot = (lax.broadcasted_iota(jnp.int32, (2 * CLIP, LINE), 0) == distance).astype(F32)
    far = (distance[:1] == 2 * CLIP).astype(F32)
    for l in range(LAYERS):
        table = rel_bias[l]
        line = jnp.dot(
            table[:, : 2 * CLIP], onehot, precision=lax.Precision.HIGHEST, preferred_element_type=F32
        ) + table[:, 2 * CLIP :] * far
        for h in range(heads):
            spread = jnp.broadcast_to(line[h : h + 1], (SEG, LINE))
            turned = pltpu.roll(spread, LINE - (SEG - 1), 1, stride=1, stride_axis=0)
            bias[l, h * SEG : (h + 1) * SEG, :] = turned

    for kv in range(kv_heads):
        vdup[kv, :, 128:] = jnp.ones((2 * row_count, 128), BF16)

    at_edge = jnp.logical_or(me_sp == 0, me_sp == n_sp - 1)

    @pl.when(at_edge)
    def _():
        pl.semaphore_wait(barrier, n_x + min(n_sp - 1, 1))

    @pl.when(jnp.logical_not(at_edge))
    def _():
        pl.semaphore_wait(barrier, n_x + 2)

    def keys_values(l, rows_in):
        both = jnp.concatenate([wk[l], wv[l]], axis=1)
        flat = jnp.dot(rows_in, both, preferred_element_type=F32)
        keys = head_norm(flat[:, :kv_width], key_gain[l : l + 1], 1.0)
        return keys, flat[:, kv_width:].astype(BF16)

    def make_queries(l, rows_in):
        flat = jnp.dot(rows_in, wq[l], preferred_element_type=F32)
        return head_norm(flat, query_gain[l : l + 1], HEAD_DIM ** (-0.5))

    def put_dup(keys, values, rows):
        for kv in range(kv_heads):
            cols = slice(kv * HEAD_DIM, (kv + 1) * HEAD_DIM)
            kdup[kv, rows, :] = jnp.concatenate([keys[:, cols]] * 2, axis=1)
            vdup[kv, rows, :128] = jnp.concatenate([values[:, cols]] * 2, axis=1)

    def halo_copy(l, seg):
        rows = seg_rows(seg)
        return send(
            pair_made.at[l, rows],
            halo.at[l, rows],
            hs_sem.at[l, seg],
            hr_sem.at[l, seg],
            {"sp": lax.rem(me_sp + 1, n_sp)},
        )

    def start_halo(l, which):
        @pl.when(me_sp < n_sp - 1)
        def _():
            for seg in which:
                halo_copy(l, seg).start()

    def finish_halo(l):
        @pl.when(me_sp > 0)
        def _():
            for seg in range(segs):
                halo_copy(l, seg).wait_recv()
            got = halo[l]
            put_dup(got[:, :kv_width], got[:, kv_width:], slice(0, row_count))

        @pl.when(me_sp == 0)
        def _():
            none = jnp.zeros((row_count, kv_width), BF16)
            put_dup(none, none, slice(0, row_count))

    def end_halo_sends(l):
        @pl.when(me_sp < n_sp - 1)
        def _():
            for seg in range(segs):
                halo_copy(l, seg).wait_send()

    lane = lax.broadcasted_iota(jnp.int32, (SEG, 128), 1)
    low_half = lane < HEAD_DIM

    def attend(l, seg):
        rows = seg_rows(seg)
        window = pl.ds(pl.multiple_of(seg * SEG, SEG), SPAN)
        key_pos = lax.broadcasted_iota(jnp.int32, (1, SPAN), 1)
        inside = me_sp * row_count + (seg - LEFT) * SEG + key_pos >= 0
        shut = jnp.where(inside, 0.0, masked_score)
        for kv in range(kv_heads):
            stack = []
            for p in range(group // 2):
                lower = (kv * group + 2 * p) * HEAD_DIM
                tile = queries[rows, lower : lower + 128]
                none = jnp.zeros_like(tile)
                stack += [jnp.where(low_half, tile, none), jnp.where(low_half, none, tile)]
            stacked = jnp.concatenate(stack, axis=0)
            scores = lax.dot_general(
                stacked, kdup[kv, window, :], (((1,), (1,)), ((), ())), preferred_element_type=F32
            )
            base = kv * group * SEG
            scores = scores + bias[l, base : base + group * SEG, :SPAN] + shut
            peak = jnp.max(scores, axis=-1, keepdims=True)
            expon = jnp.exp(scores - peak).astype(BF16)
            summed = jnp.dot(expon, vdup[kv, window, :], preferred_element_type=F32)
            made = summed[:, :128] / summed[:, 128:]
            for p in range(group // 2):
                lower = (kv * group + 2 * p) * HEAD_DIM
                even = made[2 * p * SEG : (2 * p + 1) * SEG]
                odd = made[(2 * p + 1) * SEG : (2 * p + 2) * SEG]
                mixed[:, lower : lower + 128] = jnp.where(low_half, even, odd).astype(BF16)

    def project_out(l, lower, size):
        cols = pl.ds(pl.multiple_of(lower, 128), size)
        return jnp.dot(mixed[...], wo[l, :, cols], preferred_element_type=F32)

    stream_load.wait()
    normed[...] = row_norm(cur0[...].astype(F32), attn_gain[0:1])
    weight_loads[0][0].wait()
    weight_loads[0][1].wait()
    keys, values = keys_values(0, normed[...])
    pair_made[0] = jnp.concatenate([keys, values], axis=1)
    start_halo(0, range(segs))
    put_dup(keys, values, slice(row_count, 2 * row_count))
    weight_loads[0][2].wait()
    queries[...] = make_queries(0, normed[...])
    weight_loads[0][3].wait()
    finish_halo(0)

    def partner_copy(i):
        return send(psend.at[i], precv.at[i], ps_sem.at[i], pr_sem.at[i], partner)

    def chip_copy(i, k):
        return send(
            xsend.at[i], xrecv.at[k - 1, i], xs_sem.at[k - 1, i], xr_sem.at[k - 1, i], peer(k)
        )

    def rows_copy(i):
        rows = seg_rows(core * half + i)
        return send(cur1.at[rows], cur1.at[rows], cs_sem.at[i], cr_sem.at[i], partner)

    out_step = min(width, 512)

    def first_out(i, carry):
        attend(0, (1 - core) * half + i)
        for lower in range(0, width, out_step):
            psend[i, :, lower : lower + out_step] = project_out(0, lower, out_step).astype(BF16)
        partner_copy(i).start()
        attend(0, core * half + i)
        for lower in range(0, width, out_step):
            own0[i, :, lower : lower + out_step] = project_out(0, lower, out_step)
        partner_copy(i).wait_recv()
        both = own0[i] + precv[i].astype(F32)
        own0[i] = both
        xsend[i] = both.astype(BF16)
        for k in range(1, n_x):
            chip_copy(i, k).start()
        return carry

    lax.fori_loop(0, half, first_out, 0)

    for l in range(1, LAYERS):
        for copy in weight_loads[l]:
            copy.wait()

    for i in range(half):
        mine = core * half + i
        theirs = (1 - core) * half + i
        total = own0[i]
        for k in range(1, n_x):
            chip_copy(i, k).wait_recv()
            total = total + xrecv[k - 1, i].astype(F32)
        cur1[seg_rows(mine), :] = (cur0[seg_rows(mine), :].astype(F32) + total).astype(BF16)
        rows_copy(i).start()
        normed[0:SEG, :] = row_norm(cur1[seg_rows(mine), :].astype(F32), attn_gain[1:2])
        send(
            cur1.at[seg_rows(theirs)], cur1.at[seg_rows(theirs)], cs_sem.at[i], cr_sem.at[i], partner
        ).wait_recv()
        normed[SEG : 2 * SEG, :] = row_norm(cur1[seg_rows(theirs), :].astype(F32), attn_gain[1:2])
        rows_in = normed[0 : 2 * SEG, :]
        keys, values = keys_values(1, rows_in)
        made = jnp.concatenate([keys, values], axis=1)
        for n, seg in enumerate((mine, theirs)):
            part = slice(n * SEG, (n + 1) * SEG)
            pair_made[1, seg_rows(seg), :] = made[part]
        start_halo(1, (mine, theirs))
        for n, seg in enumerate((mine, theirs)):
            part = slice(n * SEG, (n + 1) * SEG)
            put_dup(keys[part], values[part], seg_rows(seg + segs))
        made_q = make_queries(1, rows_in)
        for n, seg in enumerate((mine, theirs)):
            queries[seg_rows(seg), :] = made_q[n * SEG : (n + 1) * SEG]
    finish_halo(1)

    def partner_copy1(s):
        return send(psend1.at[s], precv1.at[s], ps1_sem.at[s], pr1_sem.at[s], partner)

    def chip_copy1(s, k):
        return send(
            xsend1.at[k - 1, s],
            xrecv1.at[k - 1, s],
            xs1_sem.at[k - 1, s],
            xr1_sem.at[k - 1, s],
            peer(k),
        )

    def last_sends(s):
        partner_copy1(s).wait_recv()
        for k in range(n_x):
            both = own1[s, k] + precv1[s, k].astype(F32)
            if k == 0:
                own1[s, k] = both
            else:
                xsend1[k - 1, s] = both.astype(BF16)
                chip_copy1(s, k).start()

    def last_out(s, carry):
        attend(1, s)
        for k in range(n_x):
            lower = (chip_at(k) * 2 + 1 - core) * feat
            psend1[s, k] = project_out(1, lower, feat).astype(BF16)
        partner_copy1(s).start()
        for k in range(n_x):
            lower = (chip_at(k) * 2 + core) * feat
            own1[s, k] = project_out(1, lower, feat)

        @pl.when(s > 0)
        def _():
            last_sends(s - 1)

        return carry

    lax.fori_loop(0, segs, last_out, 0)
    last_sends(segs - 1)
    my_cols = pl.ds(pl.multiple_of(me_tp * feat, 128), feat)
    for s in range(segs):
        rows = slice(s * SEG, (s + 1) * SEG)
        total = own1[s, 0]
        for k in range(1, n_x):
            chip_copy1(s, k).wait_recv()
            total = total + xrecv1[k - 1, s].astype(F32)
        out[rows, :] = (cur1[rows, my_cols].astype(F32) + total).astype(BF16)

    for i in range(half):
        partner_copy(i).wait_send()
        rows_copy(i).wait_send()
        for k in range(1, n_x):
            chip_copy(i, k).wait_send()
    for s in range(segs):
        partner_copy1(s).wait_send()
        for k in range(1, n_x):
            chip_copy1(s, k).wait_send()
    for l in range(LAYERS):
        end_halo_sends(l)


def local(n_sp, n_tp, stream, attn_gain, w_query, w_key, w_value, w_out, query_gain, key_gain, rel_bias):
    row_count, width = stream.shape
    segs = row_count // SEG
    assert row_count == LEFT * SEG and n_tp % 2 == 0
    half = segs // 2
    n_x = n_tp // 2
    feat = width // n_tp
    q_width = w_query.shape[2]
    kv_width = w_key.shape[2]
    kv_heads = kv_width // HEAD_DIM
    heads = q_width // HEAD_DIM
    others = max(n_x - 1, 1)
    dma = pltpu.SemaphoreType.DMA
    anyw = pl.BlockSpec(memory_space=pl.ANY)
    vmem = pl.BlockSpec(memory_space=pltpu.VMEM)
    scratch = [
        pltpu.VMEM((row_count, width), BF16),
        pltpu.VMEM((row_count, width), BF16),
        pltpu.VMEM((row_count, width), BF16),
        pltpu.VMEM(w_query.shape, BF16),
        pltpu.VMEM(w_key.shape, BF16),
        pltpu.VMEM(w_value.shape, BF16),
        pltpu.VMEM(w_out.shape, BF16),
        pltpu.VMEM((row_count, q_width), BF16),
        pltpu.VMEM((LAYERS, row_count, 2 * kv_width), BF16),
        pltpu.VMEM((LAYERS, row_count, 2 * kv_width), BF16),
        pltpu.VMEM((kv_heads, 2 * row_count, 128), BF16),
        pltpu.VMEM((kv_heads, 2 * row_count, 256), BF16),
        pltpu.VMEM((LAYERS, heads * SEG, LINE), F32),
        pltpu.VMEM((SEG, q_width), BF16),
        pltpu.VMEM((half, SEG, width), BF16),
        pltpu.VMEM((half, SEG, width), BF16),
        pltpu.VMEM((half, SEG, width), F32),
        pltpu.VMEM((half, SEG, width), BF16),
        pltpu.VMEM((others, half, SEG, width), BF16),
        pltpu.VMEM((segs, n_x, SEG, feat), BF16),
        pltpu.VMEM((segs, n_x, SEG, feat), BF16),
        pltpu.VMEM((segs, n_x, SEG, feat), F32),
        pltpu.VMEM((others, segs, SEG, feat), BF16),
        pltpu.VMEM((others, segs, SEG, feat), BF16),
        dma((1 + 4 * LAYERS,)),
        dma((half,)), dma((half,)),
        dma((others, half)), dma((others, half)),
        dma((half,)), dma((half,)),
        dma((LAYERS, segs)), dma((LAYERS, segs)),
        dma((segs,)), dma((segs,)),
        dma((others, segs)), dma((others, segs)),
    ]
    return pl.pallas_call(
        functools.partial(body, n_sp, n_tp),
        out_shape=jax.ShapeDtypeStruct((row_count, feat), BF16),
        in_specs=[anyw, vmem, anyw, anyw, anyw, anyw, vmem, vmem, vmem],
        out_specs=vmem,
        scratch_shapes=scratch,
        compiler_params=pltpu.CompilerParams(
            collective_id=0, has_side_effects=True, vmem_limit_bytes=60 * 1024 * 1024
        ),
    )(stream, attn_gain, w_query, w_key, w_value, w_out, query_gain, key_gain, rel_bias)


def solution(mesh):
    return jax.shard_map(
        functools.partial(local, mesh.shape["sp"], mesh.shape["tp"]),
        mesh=mesh,
        in_specs=(
            P("sp", None),
            P(),
            P(None, None, "tp"),
            P(None, None, "tp"),
            P(None, None, "tp"),
            P(None, "tp", None),
            P(),
            P(),
            P(None, "tp", None),
        ),
        out_specs=P("sp", "tp"),
        check_vma=False,
    )
```

```python
import functools

import jax
import jax.numpy as jnp
from jax import lax
from jax.experimental import pallas as pl
from jax.experimental.pallas import tpu as pltpu
from jax.sharding import PartitionSpec as P

HEAD_DIM = 64
SEG = 64
LEFT = 4
CLIP = 128
LAYERS = 2
SPAN = (LEFT + 1) * SEG
LINE = 384

norm_eps = 1e-06
masked_score = -1e30
F32 = jnp.float32
BF16 = jnp.bfloat16


def seg_rows(seg):
    return pl.ds(pl.multiple_of(seg * SEG, SEG), SEG)


def send(src, dst, send_sem, recv_sem, device):
    return pltpu.make_async_remote_copy(
        src_ref=src,
        dst_ref=dst,
        send_sem=send_sem,
        recv_sem=recv_sem,
        device_id=device,
        device_id_type=pl.DeviceIdType.MESH,
    )


def row_norm(x, gain):
    squared = jnp.mean(x * x, axis=-1, keepdims=True)
    return (x * lax.rsqrt(squared + norm_eps) * gain).astype(BF16)


def head_norm(x, gain_row, scale):
    width = x.shape[1]
    block = min(width, 256)
    row_head = lax.broadcasted_iota(jnp.int32, (block, block), 0) >> 6
    col_head = lax.broadcasted_iota(jnp.int32, (block, block), 1) >> 6
    spread = jnp.where(row_head == col_head, 1.0 / HEAD_DIM, 0.0).astype(BF16)
    gain = jnp.concatenate([gain_row] * (block // HEAD_DIM), axis=1) * scale
    outs = []
    for lower in range(0, width, block):
        part = x[:, lower : lower + block]
        squares = part * part
        high = squares.astype(BF16)
        low = (squares - high.astype(F32)).astype(BF16)
        mean = jnp.dot(high, spread, preferred_element_type=F32) + jnp.dot(
            low, spread, preferred_element_type=F32
        )
        outs.append((part * lax.rsqrt(mean + norm_eps) * gain).astype(BF16))
    return outs[0] if len(outs) == 1 else jnp.concatenate(outs, axis=1)


def body(
    n_sp, n_tp,
    stream, attn_gain_in, w_query, w_key, w_value, w_out, query_gain_in, key_gain_in, rel_bias_in,
    out,
    attn_gain, query_gain, key_gain, rel_bias,
    cur0, cur1, normed, wq, wk, wv, wo, queries, pair_made, halo, kdup, vdup, bias, mixed,
    psend, precv, own0, xsend, xrecv,
    psend1, precv1, own1, xsend1, xrecv1,
    w_sem, ps_sem, pr_sem, xs_sem, xr_sem, cs_sem, cr_sem, hs_sem, hr_sem,
    ps1_sem, pr1_sem, xs1_sem, xr1_sem,
):
    row_count, width = cur0.shape
    segs = row_count // SEG
    half = segs // 2
    q_width = wq.shape[2]
    kv_width = wk.shape[2]
    heads = q_width // HEAD_DIM
    kv_heads = kv_width // HEAD_DIM
    group = heads // kv_heads
    n_x = n_tp // 2
    feat = width // n_tp
    me_sp = lax.axis_index("sp")
    me_tp = lax.axis_index("tp")
    core = lax.rem(me_tp, 2)
    chip = lax.div(me_tp, 2)
    partner = {"tp": chip * 2 + 1 - core}

    def chip_at(k):
        return lax.rem(chip + k, n_x)

    def peer(k):
        return {"tp": chip_at(k) * 2 + core}

    barrier = pltpu.get_barrier_semaphore()
    pl.semaphore_signal(barrier, inc=1, device_id=partner, device_id_type=pl.DeviceIdType.MESH)
    for k in range(1, n_x):
        pl.semaphore_signal(barrier, inc=1, device_id=peer(k), device_id_type=pl.DeviceIdType.MESH)

    @pl.when(me_sp > 0)
    def _():
        pl.semaphore_signal(
            barrier, inc=1, device_id={"sp": me_sp - 1}, device_id_type=pl.DeviceIdType.MESH
        )

    @pl.when(me_sp < n_sp - 1)
    def _():
        pl.semaphore_signal(
            barrier, inc=1, device_id={"sp": me_sp + 1}, device_id_type=pl.DeviceIdType.MESH
        )

    loads = []

    def load(src, dst):
        copy = pltpu.make_async_copy(src, dst, w_sem.at[len(loads)])
        copy.start()
        loads.append(copy)
        return copy

    stream_load = load(stream, cur0)
    gain_loads = [
        load(attn_gain_in, attn_gain),
        load(query_gain_in, query_gain),
        load(key_gain_in, key_gain),
        load(rel_bias_in, rel_bias),
    ]
    weight_loads = []
    for l in range(LAYERS):
        weight_loads.append(
            [
                load(w_key.at[l], wk.at[l]),
                load(w_value.at[l], wv.at[l]),
                load(w_query.at[l], wq.at[l]),
                load(w_out.at[l], wo.at[l]),
            ]
        )

    def build_bias(l):
        offset = lax.broadcasted_iota(jnp.int32, (2 * CLIP, LINE), 1)
        distance = jnp.clip(LEFT * SEG + SEG - 1 - offset, -CLIP, CLIP) + CLIP
        onehot = (lax.broadcasted_iota(jnp.int32, (2 * CLIP, LINE), 0) == distance).astype(F32)
        far = (distance[:1] == 2 * CLIP).astype(F32)
        table = rel_bias[l]
        line = jnp.dot(
            table[:, : 2 * CLIP], onehot, precision=lax.Precision.HIGHEST, preferred_element_type=F32
        ) + table[:, 2 * CLIP :] * far
        for h in range(heads):
            spread = jnp.broadcast_to(line[h : h + 1], (SEG, LINE))
            turned = pltpu.roll(spread, LINE - (SEG - 1), 1, stride=1, stride_axis=0)
            bias[l, h * SEG : (h + 1) * SEG, :] = turned

    for kv in range(kv_heads):
        vdup[kv, :, 128:] = jnp.ones((2 * row_count, 128), BF16)

    def keys_values(l, rows_in):
        both = jnp.concatenate([wk[l], wv[l]], axis=1)
        flat = jnp.dot(rows_in, both, preferred_element_type=F32)
        keys = head_norm(flat[:, :kv_width], key_gain[l : l + 1], 1.0)
        return keys, flat[:, kv_width:].astype(BF16)

    def make_queries(l, rows_in):
        flat = jnp.dot(rows_in, wq[l], preferred_element_type=F32)
        return head_norm(flat, query_gain[l : l + 1], HEAD_DIM ** (-0.5))

    def put_dup(keys, values, rows):
        for kv in range(kv_heads):
            cols = slice(kv * HEAD_DIM, (kv + 1) * HEAD_DIM)
            kdup[kv, rows, :] = jnp.concatenate([keys[:, cols]] * 2, axis=1)
            vdup[kv, rows, :128] = jnp.concatenate([values[:, cols]] * 2, axis=1)

    def halo_copy(l, seg):
        rows = seg_rows(seg)
        return send(
            pair_made.at[l, rows],
            halo.at[l, rows],
            hs_sem.at[l, seg],
            hr_sem.at[l, seg],
            {"sp": lax.rem(me_sp + 1, n_sp)},
        )

    def start_halo(l, which):
        @pl.when(me_sp < n_sp - 1)
        def _():
            for seg in which:
                halo_copy(l, seg).start()

    def finish_halo(l, seg):
        @pl.when(me_sp > 0)
        def _():
            halo_copy(l, seg).wait_recv()
            got = halo[l, seg_rows(seg), :]
            put_dup(got[:, :kv_width], got[:, kv_width:], seg_rows(seg))

        @pl.when(me_sp == 0)
        def _():
            none = jnp.zeros((SEG, kv_width), BF16)
            put_dup(none, none, seg_rows(seg))

    def end_halo_sends(l):
        @pl.when(me_sp < n_sp - 1)
        def _():
            for seg in range(segs):
                halo_copy(l, seg).wait_send()

    lane = lax.broadcasted_iota(jnp.int32, (SEG, 128), 1)
    low_half = lane < HEAD_DIM

    def attend(l, seg):
        rows = seg_rows(seg)
        window = pl.ds(pl.multiple_of(seg * SEG, SEG), SPAN)
        key_pos = lax.broadcasted_iota(jnp.int32, (1, SPAN), 1)
        inside = me_sp * row_count + (seg - LEFT) * SEG + key_pos >= 0
        shut = jnp.where(inside, 0.0, masked_score)
        for kv in range(kv_heads):
            stack = []
            for p in range(group // 2):
                lower = (kv * group + 2 * p) * HEAD_DIM
                tile = queries[rows, lower : lower + 128]
                none = jnp.zeros_like(tile)
                stack += [jnp.where(low_half, tile, none), jnp.where(low_half, none, tile)]
            stacked = jnp.concatenate(stack, axis=0)
            scores = lax.dot_general(
                stacked, kdup[kv, window, :], (((1,), (1,)), ((), ())), preferred_element_type=F32
            )
            base = kv * group * SEG
            scores = scores + bias[l, base : base + group * SEG, :SPAN] + shut
            peak = jnp.max(scores, axis=-1, keepdims=True)
            expon = jnp.exp(scores - peak).astype(BF16)
            summed = jnp.dot(expon, vdup[kv, window, :], preferred_element_type=F32)
            made = summed[:, :128] / summed[:, 128:]
            for p in range(group // 2):
                lower = (kv * group + 2 * p) * HEAD_DIM
                even = made[2 * p * SEG : (2 * p + 1) * SEG]
                odd = made[(2 * p + 1) * SEG : (2 * p + 2) * SEG]
                mixed[:, lower : lower + 128] = jnp.where(low_half, even, odd).astype(BF16)

    def project_out(l, lower, size):
        cols = pl.ds(pl.multiple_of(lower, 128), size)
        return jnp.dot(mixed[...], wo[l, :, cols], preferred_element_type=F32)

    stream_load.wait()
    for copy in gain_loads:
        copy.wait()
    normed[...] = row_norm(cur0[...].astype(F32), attn_gain[0:1])
    weight_loads[0][0].wait()
    weight_loads[0][1].wait()
    keys, values = keys_values(0, normed[...])
    pair_made[0] = jnp.concatenate([keys, values], axis=1)
    at_edge = jnp.logical_or(me_sp == 0, me_sp == n_sp - 1)

    @pl.when(at_edge)
    def _():
        pl.semaphore_wait(barrier, n_x + min(n_sp - 1, 1))

    @pl.when(jnp.logical_not(at_edge))
    def _():
        pl.semaphore_wait(barrier, n_x + 2)

    start_halo(0, reversed(range(segs)))
    put_dup(keys, values, slice(row_count, 2 * row_count))
    weight_loads[0][2].wait()
    queries[...] = make_queries(0, normed[...])
    build_bias(0)
    build_bias(1)
    weight_loads[0][3].wait()

    def mine_at(i):
        return (half - 1 - i) * 2 + core

    def theirs_at(i):
        return (half - 1 - i) * 2 + 1 - core

    def partner_copy(i):
        return send(psend.at[i], precv.at[i], ps_sem.at[i], pr_sem.at[i], partner)

    def chip_copy(i, k):
        return send(
            xsend.at[i], xrecv.at[k - 1, i], xs_sem.at[k - 1, i], xr_sem.at[k - 1, i], peer(k)
        )

    def rows_copy(i):
        rows = seg_rows(mine_at(i))
        return send(cur1.at[rows], cur1.at[rows], cs_sem.at[i], cr_sem.at[i], partner)

    out_step = min(width, 512)

    def first_out(i, carry):
        finish_halo(0, (half - 1 - i) * 2 + 1)
        finish_halo(0, (half - 1 - i) * 2)
        attend(0, theirs_at(i))
        for lower in range(0, width, out_step):
            psend[i, :, lower : lower + out_step] = project_out(0, lower, out_step).astype(BF16)
        partner_copy(i).start()
        attend(0, mine_at(i))
        for lower in range(0, width, out_step):
            own0[i, :, lower : lower + out_step] = project_out(0, lower, out_step)
        partner_copy(i).wait_recv()
        both = own0[i] + precv[i].astype(F32)
        own0[i] = both
        xsend[i] = both.astype(BF16)
        for k in range(1, n_x):
            chip_copy(i, k).start()
        return carry

    lax.fori_loop(0, half, first_out, 0)

    for l in range(1, LAYERS):
        for copy in weight_loads[l]:
            copy.wait()

    for i in range(half):
        mine = mine_at(i)
        theirs = theirs_at(i)
        total = own0[i]
        for k in range(1, n_x):
            chip_copy(i, k).wait_recv()
            total = total + xrecv[k - 1, i].astype(F32)
        cur1[seg_rows(mine), :] = (cur0[seg_rows(mine), :].astype(F32) + total).astype(BF16)
        rows_copy(i).start()
        normed[0:SEG, :] = row_norm(cur1[seg_rows(mine), :].astype(F32), attn_gain[1:2])
        send(
            cur1.at[seg_rows(theirs)], cur1.at[seg_rows(theirs)], cs_sem.at[i], cr_sem.at[i], partner
        ).wait_recv()
        normed[SEG : 2 * SEG, :] = row_norm(cur1[seg_rows(theirs), :].astype(F32), attn_gain[1:2])
        rows_in = normed[0 : 2 * SEG, :]
        keys, values = keys_values(1, rows_in)
        made = jnp.concatenate([keys, values], axis=1)
        for n, seg in enumerate((mine, theirs)):
            part = slice(n * SEG, (n + 1) * SEG)
            pair_made[1, seg_rows(seg), :] = made[part]
        start_halo(1, (mine, theirs))
        for n, seg in enumerate((mine, theirs)):
            part = slice(n * SEG, (n + 1) * SEG)
            put_dup(keys[part], values[part], seg_rows(seg + segs))
        made_q = make_queries(1, rows_in)
        for n, seg in enumerate((mine, theirs)):
            queries[seg_rows(seg), :] = made_q[n * SEG : (n + 1) * SEG]

    def partner_copy1(s):
        return send(psend1.at[s], precv1.at[s], ps1_sem.at[s], pr1_sem.at[s], partner)

    def chip_copy1(s, k):
        return send(
            xsend1.at[k - 1, s],
            xrecv1.at[k - 1, s],
            xs1_sem.at[k - 1, s],
            xr1_sem.at[k - 1, s],
            peer(k),
        )

    def last_sends(s):
        partner_copy1(s).wait_recv()
        for k in range(n_x):
            both = own1[s, k] + precv1[s, k].astype(F32)
            if k == 0:
                own1[s, k] = both
            else:
                xsend1[k - 1, s] = both.astype(BF16)
                chip_copy1(s, k).start()

    def last_out(s, carry):
        finish_halo(1, segs - 1 - s)
        attend(1, segs - 1 - s)
        for k in range(n_x):
            lower = (chip_at(k) * 2 + 1 - core) * feat
            psend1[s, k] = project_out(1, lower, feat).astype(BF16)
        partner_copy1(s).start()
        for k in range(n_x):
            lower = (chip_at(k) * 2 + core) * feat
            own1[s, k] = project_out(1, lower, feat)

        @pl.when(s > 0)
        def _():
            last_sends(s - 1)

        return carry

    lax.fori_loop(0, segs, last_out, 0)
    last_sends(segs - 1)
    my_cols = pl.ds(pl.multiple_of(me_tp * feat, 128), feat)
    for s in range(segs):
        rows = slice((segs - 1 - s) * SEG, (segs - s) * SEG)
        total = own1[s, 0]
        for k in range(1, n_x):
            chip_copy1(s, k).wait_recv()
            total = total + xrecv1[k - 1, s].astype(F32)
        out[rows, :] = (cur1[rows, my_cols].astype(F32) + total).astype(BF16)

    for i in range(half):
        partner_copy(i).wait_send()
        rows_copy(i).wait_send()
        for k in range(1, n_x):
            chip_copy(i, k).wait_send()
    for s in range(segs):
        partner_copy1(s).wait_send()
        for k in range(1, n_x):
            chip_copy1(s, k).wait_send()
    for l in range(LAYERS):
        end_halo_sends(l)


def local(n_sp, n_tp, stream, attn_gain, w_query, w_key, w_value, w_out, query_gain, key_gain, rel_bias):
    row_count, width = stream.shape
    segs = row_count // SEG
    assert row_count == LEFT * SEG and n_tp % 2 == 0
    half = segs // 2
    n_x = n_tp // 2
    feat = width // n_tp
    q_width = w_query.shape[2]
    kv_width = w_key.shape[2]
    kv_heads = kv_width // HEAD_DIM
    heads = q_width // HEAD_DIM
    others = max(n_x - 1, 1)
    dma = pltpu.SemaphoreType.DMA
    anyw = pl.BlockSpec(memory_space=pl.ANY)
    vmem = pl.BlockSpec(memory_space=pltpu.VMEM)
    scratch = [
        pltpu.VMEM(attn_gain.shape, F32),
        pltpu.VMEM(query_gain.shape, F32),
        pltpu.VMEM(key_gain.shape, F32),
        pltpu.VMEM(rel_bias.shape, F32),
        pltpu.VMEM((row_count, width), BF16),
        pltpu.VMEM((row_count, width), BF16),
        pltpu.VMEM((row_count, width), BF16),
        pltpu.VMEM(w_query.shape, BF16),
        pltpu.VMEM(w_key.shape, BF16),
        pltpu.VMEM(w_value.shape, BF16),
        pltpu.VMEM(w_out.shape, BF16),
        pltpu.VMEM((row_count, q_width), BF16),
        pltpu.VMEM((LAYERS, row_count, 2 * kv_width), BF16),
        pltpu.VMEM((LAYERS, row_count, 2 * kv_width), BF16),
        pltpu.VMEM((kv_heads, 2 * row_count, 128), BF16),
        pltpu.VMEM((kv_heads, 2 * row_count, 256), BF16),
        pltpu.VMEM((LAYERS, heads * SEG, LINE), F32),
        pltpu.VMEM((SEG, q_width), BF16),
        pltpu.VMEM((half, SEG, width), BF16),
        pltpu.VMEM((half, SEG, width), BF16),
        pltpu.VMEM((half, SEG, width), F32),
        pltpu.VMEM((half, SEG, width), BF16),
        pltpu.VMEM((others, half, SEG, width), BF16),
        pltpu.VMEM((segs, n_x, SEG, feat), BF16),
        pltpu.VMEM((segs, n_x, SEG, feat), BF16),
        pltpu.VMEM((segs, n_x, SEG, feat), F32),
        pltpu.VMEM((others, segs, SEG, feat), BF16),
        pltpu.VMEM((others, segs, SEG, feat), BF16),
        dma((5 + 4 * LAYERS,)),
        dma((half,)), dma((half,)),
        dma((others, half)), dma((others, half)),
        dma((half,)), dma((half,)),
        dma((LAYERS, segs)), dma((LAYERS, segs)),
        dma((segs,)), dma((segs,)),
        dma((others, segs)), dma((others, segs)),
    ]
    return pl.pallas_call(
        functools.partial(body, n_sp, n_tp),
        out_shape=jax.ShapeDtypeStruct((row_count, feat), BF16),
        in_specs=[anyw] * 9,
        out_specs=vmem,
        scratch_shapes=scratch,
        compiler_params=pltpu.CompilerParams(
            collective_id=0, has_side_effects=True, vmem_limit_bytes=60 * 1024 * 1024
        ),
    )(stream, attn_gain, w_query, w_key, w_value, w_out, query_gain, key_gain, rel_bias)


def solution(mesh):
    return jax.shard_map(
        functools.partial(local, mesh.shape["sp"], mesh.shape["tp"]),
        mesh=mesh,
        in_specs=(
            P("sp", None),
            P(),
            P(None, None, "tp"),
            P(None, None, "tp"),
            P(None, None, "tp"),
            P(None, "tp", None),
            P(),
            P(),
            P(None, "tp", None),
        ),
        out_specs=P("sp", "tp"),
        check_vma=False,
    )
```

```python
import functools

import jax
import jax.numpy as jnp
from jax import lax
from jax.experimental import pallas as pl
from jax.experimental.pallas import tpu as pltpu
from jax.sharding import PartitionSpec as P

HEAD_DIM = 64
SEG = 64
LEFT = 4
CLIP = 128
LAYERS = 2
SPAN = (LEFT + 1) * SEG
LINE = 384
SUBS = 2

norm_eps = 1e-06
masked_score = -1e30
F32 = jnp.float32
BF16 = jnp.bfloat16


def seg_rows(seg):
    return pl.ds(pl.multiple_of(seg * SEG, SEG), SEG)


def send(src, dst, send_sem, recv_sem, device):
    return pltpu.make_async_remote_copy(
        src_ref=src,
        dst_ref=dst,
        send_sem=send_sem,
        recv_sem=recv_sem,
        device_id=device,
        device_id_type=pl.DeviceIdType.MESH,
    )


def row_norm(x, gain):
    squared = jnp.mean(x * x, axis=-1, keepdims=True)
    return (x * lax.rsqrt(squared + norm_eps) * gain).astype(BF16)


def head_norm(x, gain_row, scale):
    width = x.shape[1]
    block = min(width, 256)
    row_head = lax.broadcasted_iota(jnp.int32, (block, block), 0) >> 6
    col_head = lax.broadcasted_iota(jnp.int32, (block, block), 1) >> 6
    spread = jnp.where(row_head == col_head, 1.0 / HEAD_DIM, 0.0).astype(BF16)
    gain = jnp.concatenate([gain_row] * (block // HEAD_DIM), axis=1) * scale
    outs = []
    for lower in range(0, width, block):
        part = x[:, lower : lower + block]
        squares = part * part
        high = squares.astype(BF16)
        low = (squares - high.astype(F32)).astype(BF16)
        mean = jnp.dot(high, spread, preferred_element_type=F32) + jnp.dot(
            low, spread, preferred_element_type=F32
        )
        outs.append((part * lax.rsqrt(mean + norm_eps) * gain).astype(BF16))
    return outs[0] if len(outs) == 1 else jnp.concatenate(outs, axis=1)


def body(
    n_sp, n_tp,
    stream, attn_gain_in, w_query, w_key, w_value, w_out, query_gain_in, key_gain_in, rel_bias_in,
    out,
    attn_gain, query_gain, key_gain, rel_bias,
    cur0, cur1, normed, wq, wk, wv, wo, queries, pair_made, halo, kdup, vdup, bias, mixed,
    psend, precv, own0, xsend, xrecv,
    psend1, precv1, own1, xsend1, xrecv1,
    w_sem, ps_sem, pr_sem, xs_sem, xr_sem, cs_sem, cr_sem, hs_sem, hr_sem,
    ps1_sem, pr1_sem, xs1_sem, xr1_sem,
):
    row_count, width = cur0.shape
    segs = row_count // SEG
    half = segs // 2
    q_width = wq.shape[2]
    kv_width = wk.shape[2]
    heads = q_width // HEAD_DIM
    kv_heads = kv_width // HEAD_DIM
    group = heads // kv_heads
    n_x = n_tp // 2
    feat = width // n_tp
    me_sp = lax.axis_index("sp")
    me_tp = lax.axis_index("tp")
    core = lax.rem(me_tp, 2)
    chip = lax.div(me_tp, 2)
    partner = {"tp": chip * 2 + 1 - core}

    def chip_at(k):
        return lax.rem(chip + k, n_x)

    def peer(k):
        return {"tp": chip_at(k) * 2 + core}

    barrier = pltpu.get_barrier_semaphore()
    pl.semaphore_signal(barrier, inc=1, device_id=partner, device_id_type=pl.DeviceIdType.MESH)
    for k in range(1, n_x):
        pl.semaphore_signal(barrier, inc=1, device_id=peer(k), device_id_type=pl.DeviceIdType.MESH)

    @pl.when(me_sp > 0)
    def _():
        pl.semaphore_signal(
            barrier, inc=1, device_id={"sp": me_sp - 1}, device_id_type=pl.DeviceIdType.MESH
        )

    @pl.when(me_sp < n_sp - 1)
    def _():
        pl.semaphore_signal(
            barrier, inc=1, device_id={"sp": me_sp + 1}, device_id_type=pl.DeviceIdType.MESH
        )

    loads = []

    def load(src, dst):
        copy = pltpu.make_async_copy(src, dst, w_sem.at[len(loads)])
        copy.start()
        loads.append(copy)
        return copy

    part_rows = row_count // 2
    parts = [pl.ds(n * part_rows, part_rows) for n in (1, 0)]
    stream_loads = [load(stream.at[part], cur0.at[part]) for part in parts]
    gain_loads = [
        load(attn_gain_in, attn_gain),
        load(query_gain_in, query_gain),
        load(key_gain_in, key_gain),
        load(rel_bias_in, rel_bias),
    ]
    weight_loads = []
    for l in range(LAYERS):
        weight_loads.append(
            [
                load(w_key.at[l], wk.at[l]),
                load(w_value.at[l], wv.at[l]),
                load(w_query.at[l], wq.at[l]),
                load(w_out.at[l], wo.at[l]),
            ]
        )

    def build_bias(l):
        offset = lax.broadcasted_iota(jnp.int32, (2 * CLIP, LINE), 1)
        distance = jnp.clip(LEFT * SEG + SEG - 1 - offset, -CLIP, CLIP) + CLIP
        onehot = (lax.broadcasted_iota(jnp.int32, (2 * CLIP, LINE), 0) == distance).astype(F32)
        far = (distance[:1] == 2 * CLIP).astype(F32)
        table = rel_bias[l]
        line = jnp.dot(
            table[:, : 2 * CLIP], onehot, precision=lax.Precision.HIGHEST, preferred_element_type=F32
        ) + table[:, 2 * CLIP :] * far
        for h in range(heads):
            spread = jnp.broadcast_to(line[h : h + 1], (SEG, LINE))
            turned = pltpu.roll(spread, LINE - (SEG - 1), 1, stride=1, stride_axis=0)
            bias[l, h * SEG : (h + 1) * SEG, :] = turned

    for kv in range(kv_heads):
        vdup[kv, :, 128:] = jnp.ones((2 * row_count, 128), BF16)

    def keys_values(l, rows_in):
        both = jnp.concatenate([wk[l], wv[l]], axis=1)
        flat = jnp.dot(rows_in, both, preferred_element_type=F32)
        keys = head_norm(flat[:, :kv_width], key_gain[l : l + 1], 1.0)
        return keys, flat[:, kv_width:].astype(BF16)

    def make_queries(l, rows_in):
        flat = jnp.dot(rows_in, wq[l], preferred_element_type=F32)
        return head_norm(flat, query_gain[l : l + 1], HEAD_DIM ** (-0.5))

    def put_dup(keys, values, rows):
        for kv in range(kv_heads):
            cols = slice(kv * HEAD_DIM, (kv + 1) * HEAD_DIM)
            kdup[kv, rows, :] = jnp.concatenate([keys[:, cols]] * 2, axis=1)
            vdup[kv, rows, :128] = jnp.concatenate([values[:, cols]] * 2, axis=1)

    def halo_copy(l, seg):
        rows = seg_rows(seg)
        return send(
            pair_made.at[l, rows],
            halo.at[l, rows],
            hs_sem.at[l, seg],
            hr_sem.at[l, seg],
            {"sp": lax.rem(me_sp + 1, n_sp)},
        )

    def start_halo(l, which):
        @pl.when(me_sp < n_sp - 1)
        def _():
            for seg in which:
                halo_copy(l, seg).start()

    def finish_halo(l, seg):
        @pl.when(me_sp > 0)
        def _():
            halo_copy(l, seg).wait_recv()
            got = halo[l, seg_rows(seg), :]
            put_dup(got[:, :kv_width], got[:, kv_width:], seg_rows(seg))

        @pl.when(me_sp == 0)
        def _():
            none = jnp.zeros((SEG, kv_width), BF16)
            put_dup(none, none, seg_rows(seg))

    def end_halo_sends(l):
        @pl.when(me_sp < n_sp - 1)
        def _():
            for seg in range(segs):
                halo_copy(l, seg).wait_send()

    lane = lax.broadcasted_iota(jnp.int32, (SEG, 128), 1)
    low_half = lane < HEAD_DIM

    def attend(l, seg):
        rows = seg_rows(seg)
        window = pl.ds(pl.multiple_of(seg * SEG, SEG), SPAN)
        key_pos = lax.broadcasted_iota(jnp.int32, (1, SPAN), 1)
        inside = me_sp * row_count + (seg - LEFT) * SEG + key_pos >= 0
        shut = jnp.where(inside, 0.0, masked_score)
        for kv in range(kv_heads):
            stack = []
            for p in range(group // 2):
                lower = (kv * group + 2 * p) * HEAD_DIM
                tile = queries[rows, lower : lower + 128]
                none = jnp.zeros_like(tile)
                stack += [jnp.where(low_half, tile, none), jnp.where(low_half, none, tile)]
            stacked = jnp.concatenate(stack, axis=0)
            scores = lax.dot_general(
                stacked, kdup[kv, window, :], (((1,), (1,)), ((), ())), preferred_element_type=F32
            )
            base = kv * group * SEG
            scores = scores + bias[l, base : base + group * SEG, :SPAN] + shut
            peak = jnp.max(scores, axis=-1, keepdims=True)
            expon = jnp.exp(scores - peak).astype(BF16)
            summed = jnp.dot(expon, vdup[kv, window, :], preferred_element_type=F32)
            made = summed[:, :128] / summed[:, 128:]
            for p in range(group // 2):
                lower = (kv * group + 2 * p) * HEAD_DIM
                even = made[2 * p * SEG : (2 * p + 1) * SEG]
                odd = made[(2 * p + 1) * SEG : (2 * p + 2) * SEG]
                mixed[:, lower : lower + 128] = jnp.where(low_half, even, odd).astype(BF16)

    def project_out(l, lower, size):
        cols = pl.ds(pl.multiple_of(lower, 128), size)
        return jnp.dot(mixed[...], wo[l, :, cols], preferred_element_type=F32)

    def meet():
        at_edge = jnp.logical_or(me_sp == 0, me_sp == n_sp - 1)

        @pl.when(at_edge)
        def _():
            pl.semaphore_wait(barrier, n_x + min(n_sp - 1, 1))

        @pl.when(jnp.logical_not(at_edge))
        def _():
            pl.semaphore_wait(barrier, n_x + 2)

    for n, part in enumerate(parts):
        stream_loads[n].wait()
        if n == 0:
            gain_loads[0].wait()
        normed[part, :] = row_norm(cur0[part, :].astype(F32), attn_gain[0:1])
        if n == 0:
            for copy in gain_loads[1:]:
                copy.wait()
            weight_loads[0][0].wait()
            weight_loads[0][1].wait()
        keys, values = keys_values(0, normed[part, :])
        pair_made[0, part, :] = jnp.concatenate([keys, values], axis=1)
        if n == 0:
            meet()
        first_seg = (1 - n) * (segs // 2)
        start_halo(0, reversed(range(first_seg, first_seg + segs // 2)))
        put_dup(keys, values, pl.ds(row_count + (1 - n) * part_rows, part_rows))
    weight_loads[0][2].wait()
    queries[...] = make_queries(0, normed[...])
    build_bias(0)
    build_bias(1)
    weight_loads[0][3].wait()

    def mine_at(i):
        return (half - 1 - i) * 2 + core

    def theirs_at(i):
        return (half - 1 - i) * 2 + 1 - core

    def partner_copy(i):
        return send(psend.at[i], precv.at[i], ps_sem.at[i], pr_sem.at[i], partner)

    sub = SEG // SUBS

    def chip_copy(i, j, k):
        rows = pl.ds(j * sub, sub)
        return send(
            xsend.at[i, rows],
            xrecv.at[k - 1, i, rows],
            xs_sem.at[k - 1, i, j],
            xr_sem.at[k - 1, i, j],
            peer(k),
        )

    def sub_rows(seg, j):
        return pl.ds(pl.multiple_of(seg * SEG + j * sub, sub), sub)

    def rows_copy(i, j, seg):
        rows = sub_rows(seg, j)
        return send(cur1.at[rows], cur1.at[rows], cs_sem.at[i, j], cr_sem.at[i, j], partner)

    out_step = min(width, 512)

    def first_out(i, carry):
        finish_halo(0, (half - 1 - i) * 2 + 1)
        finish_halo(0, (half - 1 - i) * 2)
        attend(0, theirs_at(i))
        for lower in range(0, width, out_step):
            psend[i, :, lower : lower + out_step] = project_out(0, lower, out_step).astype(BF16)
        partner_copy(i).start()
        attend(0, mine_at(i))
        for lower in range(0, width, out_step):
            own0[i, :, lower : lower + out_step] = project_out(0, lower, out_step)
        partner_copy(i).wait_recv()
        for j in range(SUBS):
            rows = slice(j * sub, (j + 1) * sub)
            both = own0[i, rows, :] + precv[i, rows, :].astype(F32)
            own0[i, rows, :] = both
            xsend[i, rows, :] = both.astype(BF16)
            for k in range(1, n_x):
                chip_copy(i, j, k).start()
        return carry

    lax.fori_loop(0, half, first_out, 0)

    for l in range(1, LAYERS):
        for copy in weight_loads[l]:
            copy.wait()

    for i in range(half):
        mine = mine_at(i)
        theirs = theirs_at(i)
        for j in range(SUBS):
            total = own0[i, j * sub : (j + 1) * sub, :]
            for k in range(1, n_x):
                chip_copy(i, j, k).wait_recv()
                total = total + xrecv[k - 1, i, j * sub : (j + 1) * sub, :].astype(F32)
            rows = sub_rows(mine, j)
            summed = (cur0[rows, :].astype(F32) + total).astype(BF16)
            cur1[rows, :] = summed
            rows_copy(i, j, mine).start()
            normed[j * sub : (j + 1) * sub, :] = row_norm(summed.astype(F32), attn_gain[1:2])
        for j in range(SUBS):
            rows_copy(i, j, theirs).wait_recv()
            normed[SEG + j * sub : SEG + (j + 1) * sub, :] = row_norm(
                cur1[sub_rows(theirs, j), :].astype(F32), attn_gain[1:2]
            )
        rows_in = normed[0 : 2 * SEG, :]
        keys, values = keys_values(1, rows_in)
        made = jnp.concatenate([keys, values], axis=1)
        for n, seg in enumerate((mine, theirs)):
            part = slice(n * SEG, (n + 1) * SEG)
            pair_made[1, seg_rows(seg), :] = made[part]
        start_halo(1, (mine, theirs))
        for n, seg in enumerate((mine, theirs)):
            part = slice(n * SEG, (n + 1) * SEG)
            put_dup(keys[part], values[part], seg_rows(seg + segs))
        made_q = make_queries(1, rows_in)
        for n, seg in enumerate((mine, theirs)):
            queries[seg_rows(seg), :] = made_q[n * SEG : (n + 1) * SEG]

    def partner_copy1(s):
        return send(psend1.at[s], precv1.at[s], ps1_sem.at[s], pr1_sem.at[s], partner)

    def chip_copy1(s, k):
        return send(
            xsend1.at[k - 1, s],
            xrecv1.at[k - 1, s],
            xs1_sem.at[k - 1, s],
            xr1_sem.at[k - 1, s],
            peer(k),
        )

    def last_sends(s):
        partner_copy1(s).wait_recv()
        for k in range(n_x):
            both = own1[s, k] + precv1[s, k].astype(F32)
            if k == 0:
                own1[s, k] = both
            else:
                xsend1[k - 1, s] = both.astype(BF16)
                chip_copy1(s, k).start()

    def last_out(s, carry):
        finish_halo(1, segs - 1 - s)
        attend(1, segs - 1 - s)
        for k in range(n_x):
            lower = (chip_at(k) * 2 + 1 - core) * feat
            psend1[s, k] = project_out(1, lower, feat).astype(BF16)
        partner_copy1(s).start()
        for k in range(n_x):
            lower = (chip_at(k) * 2 + core) * feat
            own1[s, k] = project_out(1, lower, feat)

        @pl.when(s > 0)
        def _():
            last_sends(s - 1)

        return carry

    lax.fori_loop(0, segs, last_out, 0)
    last_sends(segs - 1)
    my_cols = pl.ds(pl.multiple_of(me_tp * feat, 128), feat)
    for s in range(segs):
        rows = slice((segs - 1 - s) * SEG, (segs - s) * SEG)
        total = own1[s, 0]
        for k in range(1, n_x):
            chip_copy1(s, k).wait_recv()
            total = total + xrecv1[k - 1, s].astype(F32)
        out[rows, :] = (cur1[rows, my_cols].astype(F32) + total).astype(BF16)

    for i in range(half):
        partner_copy(i).wait_send()
        for j in range(SUBS):
            rows_copy(i, j, mine_at(i)).wait_send()
            for k in range(1, n_x):
                chip_copy(i, j, k).wait_send()
    for s in range(segs):
        partner_copy1(s).wait_send()
        for k in range(1, n_x):
            chip_copy1(s, k).wait_send()
    for l in range(LAYERS):
        end_halo_sends(l)


def local(n_sp, n_tp, stream, attn_gain, w_query, w_key, w_value, w_out, query_gain, key_gain, rel_bias):
    row_count, width = stream.shape
    segs = row_count // SEG
    assert row_count == LEFT * SEG and n_tp % 2 == 0
    half = segs // 2
    n_x = n_tp // 2
    feat = width // n_tp
    q_width = w_query.shape[2]
    kv_width = w_key.shape[2]
    kv_heads = kv_width // HEAD_DIM
    heads = q_width // HEAD_DIM
    others = max(n_x - 1, 1)
    dma = pltpu.SemaphoreType.DMA
    anyw = pl.BlockSpec(memory_space=pltpu.HBM)
    vmem = pl.BlockSpec(memory_space=pltpu.VMEM)
    scratch = [
        pltpu.VMEM(attn_gain.shape, F32),
        pltpu.VMEM(query_gain.shape, F32),
        pltpu.VMEM(key_gain.shape, F32),
        pltpu.VMEM(rel_bias.shape, F32),
        pltpu.VMEM((row_count, width), BF16),
        pltpu.VMEM((row_count, width), BF16),
        pltpu.VMEM((row_count, width), BF16),
        pltpu.VMEM(w_query.shape, BF16),
        pltpu.VMEM(w_key.shape, BF16),
        pltpu.VMEM(w_value.shape, BF16),
        pltpu.VMEM(w_out.shape, BF16),
        pltpu.VMEM((row_count, q_width), BF16),
        pltpu.VMEM((LAYERS, row_count, 2 * kv_width), BF16),
        pltpu.VMEM((LAYERS, row_count, 2 * kv_width), BF16),
        pltpu.VMEM((kv_heads, 2 * row_count, 128), BF16),
        pltpu.VMEM((kv_heads, 2 * row_count, 256), BF16),
        pltpu.VMEM((LAYERS, heads * SEG, LINE), F32),
        pltpu.VMEM((SEG, q_width), BF16),
        pltpu.VMEM((half, SEG, width), BF16),
        pltpu.VMEM((half, SEG, width), BF16),
        pltpu.VMEM((half, SEG, width), F32),
        pltpu.VMEM((half, SEG, width), BF16),
        pltpu.VMEM((others, half, SEG, width), BF16),
        pltpu.VMEM((segs, n_x, SEG, feat), BF16),
        pltpu.VMEM((segs, n_x, SEG, feat), BF16),
        pltpu.VMEM((segs, n_x, SEG, feat), F32),
        pltpu.VMEM((others, segs, SEG, feat), BF16),
        pltpu.VMEM((others, segs, SEG, feat), BF16),
        dma((6 + 4 * LAYERS,)),
        dma((half,)), dma((half,)),
        dma((others, half, SUBS)), dma((others, half, SUBS)),
        dma((half, SUBS)), dma((half, SUBS)),
        dma((LAYERS, segs)), dma((LAYERS, segs)),
        dma((segs,)), dma((segs,)),
        dma((others, segs)), dma((others, segs)),
    ]
    return pl.pallas_call(
        functools.partial(body, n_sp, n_tp),
        out_shape=pltpu.VMEM((row_count, feat), BF16),
        in_specs=[anyw] * 9,
        out_specs=vmem,
        scratch_shapes=scratch,
        compiler_params=pltpu.CompilerParams(
            collective_id=0, has_side_effects=True, vmem_limit_bytes=60 * 1024 * 1024
        ),
    )(stream, attn_gain, w_query, w_key, w_value, w_out, query_gain, key_gain, rel_bias)


def solution(mesh):
    return jax.shard_map(
        functools.partial(local, mesh.shape["sp"], mesh.shape["tp"]),
        mesh=mesh,
        in_specs=(
            P("sp", None),
            P(),
            P(None, None, "tp"),
            P(None, None, "tp"),
            P(None, None, "tp"),
            P(None, "tp", None),
            P(),
            P(),
            P(None, "tp", None),
        ),
        out_specs=P("sp", "tp"),
        check_vma=False,
    )
```

```python
import functools

import jax
import jax.numpy as jnp
from jax import lax
from jax.experimental import pallas as pl
from jax.experimental.pallas import tpu as pltpu
from jax.sharding import PartitionSpec as P

HEAD_DIM = 64
SEG = 64
LEFT = 4
CLIP = 128
LAYERS = 2
SPAN = (LEFT + 1) * SEG
LINE = 384
SUBS = 2

norm_eps = 1e-06
masked_score = -1e30
F32 = jnp.float32
BF16 = jnp.bfloat16


def seg_rows(seg):
    return pl.ds(pl.multiple_of(seg * SEG, SEG), SEG)


def send(src, dst, send_sem, recv_sem, device):
    return pltpu.make_async_remote_copy(
        src_ref=src,
        dst_ref=dst,
        send_sem=send_sem,
        recv_sem=recv_sem,
        device_id=device,
        device_id_type=pl.DeviceIdType.MESH,
    )


def row_norm(x, gain):
    squared = jnp.mean(x * x, axis=-1, keepdims=True)
    return (x * lax.rsqrt(squared + norm_eps) * gain).astype(BF16)


def head_norm(x, gain_row, scale):
    width = x.shape[1]
    block = min(width, 256)
    row_head = lax.broadcasted_iota(jnp.int32, (block, block), 0) >> 6
    col_head = lax.broadcasted_iota(jnp.int32, (block, block), 1) >> 6
    spread = jnp.where(row_head == col_head, 1.0 / HEAD_DIM, 0.0).astype(BF16)
    gain = jnp.concatenate([gain_row] * (block // HEAD_DIM), axis=1) * scale
    outs = []
    for lower in range(0, width, block):
        part = x[:, lower : lower + block]
        squares = part * part
        high = squares.astype(BF16)
        low = (squares - high.astype(F32)).astype(BF16)
        mean = jnp.dot(high, spread, preferred_element_type=F32) + jnp.dot(
            low, spread, preferred_element_type=F32
        )
        outs.append((part * lax.rsqrt(mean + norm_eps) * gain).astype(BF16))
    return outs[0] if len(outs) == 1 else jnp.concatenate(outs, axis=1)


def body(
    n_sp, n_tp,
    stream, attn_gain_in, w_query, w_key, w_value, w_out, query_gain_in, key_gain_in, rel_bias_in,
    out,
    attn_gain, query_gain, key_gain, rel_bias,
    cur0, cur1, normed, wq, wk, wv, wo, queries, pair_made, halo, kdup, vdup, bias, mixed,
    psend, precv, own0, xsend, xrecv,
    psend1, precv1, own1, xsend1, xrecv1,
    w_sem, ps_sem, pr_sem, xs_sem, xr_sem, cs_sem, cr_sem, hs_sem, hr_sem,
    ps1_sem, pr1_sem, xs1_sem, xr1_sem,
):
    row_count, width = cur0.shape
    segs = row_count // SEG
    half = segs // 2
    q_width = wq.shape[2]
    kv_width = wk.shape[2]
    heads = q_width // HEAD_DIM
    kv_heads = kv_width // HEAD_DIM
    group = heads // kv_heads
    n_x = n_tp // 2
    feat = width // n_tp
    me_sp = lax.axis_index("sp")
    me_tp = lax.axis_index("tp")
    core = lax.rem(me_tp, 2)
    chip = lax.div(me_tp, 2)
    partner = {"tp": chip * 2 + 1 - core}

    def chip_at(k):
        return lax.rem(chip + k, n_x)

    def peer(k):
        return {"tp": chip_at(k) * 2 + core}

    barrier = pltpu.get_barrier_semaphore()
    pl.semaphore_signal(barrier, inc=1, device_id=partner, device_id_type=pl.DeviceIdType.MESH)
    for k in range(1, n_x):
        pl.semaphore_signal(barrier, inc=1, device_id=peer(k), device_id_type=pl.DeviceIdType.MESH)

    @pl.when(me_sp > 0)
    def _():
        pl.semaphore_signal(
            barrier, inc=1, device_id={"sp": me_sp - 1}, device_id_type=pl.DeviceIdType.MESH
        )

    @pl.when(me_sp < n_sp - 1)
    def _():
        pl.semaphore_signal(
            barrier, inc=1, device_id={"sp": me_sp + 1}, device_id_type=pl.DeviceIdType.MESH
        )

    loads = []

    def load(src, dst):
        copy = pltpu.make_async_copy(src, dst, w_sem.at[len(loads)])
        copy.start()
        loads.append(copy)
        return copy

    part_rows = row_count // 2
    parts = [pl.ds(n * part_rows, part_rows) for n in (1, 0)]
    stream_loads = [load(stream.at[part], cur0.at[part]) for part in parts]
    gain_loads = [
        load(attn_gain_in, attn_gain),
        load(query_gain_in, query_gain),
        load(key_gain_in, key_gain),
        load(rel_bias_in, rel_bias),
    ]
    weight_loads = []
    for l in range(LAYERS):
        weight_loads.append(
            [
                load(w_key.at[l], wk.at[l]),
                load(w_value.at[l], wv.at[l]),
                load(w_query.at[l], wq.at[l]),
                load(w_out.at[l], wo.at[l]),
            ]
        )

    def build_bias(l):
        offset = lax.broadcasted_iota(jnp.int32, (2 * CLIP, LINE), 1)
        distance = jnp.clip(LEFT * SEG + SEG - 1 - offset, -CLIP, CLIP) + CLIP
        onehot = (lax.broadcasted_iota(jnp.int32, (2 * CLIP, LINE), 0) == distance).astype(F32)
        far = (distance[:1] == 2 * CLIP).astype(F32)
        table = rel_bias[l]
        line = jnp.dot(
            table[:, : 2 * CLIP], onehot, precision=lax.Precision.HIGHEST, preferred_element_type=F32
        ) + table[:, 2 * CLIP :] * far
        for h in range(heads):
            spread = jnp.broadcast_to(line[h : h + 1], (SEG, LINE))
            turned = pltpu.roll(spread, LINE - (SEG - 1), 1, stride=1, stride_axis=0)
            bias[l, h * SEG : (h + 1) * SEG, :] = turned

    for kv in range(kv_heads):
        vdup[kv, :, 128:] = jnp.ones((2 * row_count, 128), BF16)

    def keys_values(l, rows_in):
        both = jnp.concatenate([wk[l], wv[l]], axis=1)
        flat = jnp.dot(rows_in, both, preferred_element_type=F32)
        keys = head_norm(flat[:, :kv_width], key_gain[l : l + 1], 1.0)
        return keys, flat[:, kv_width:].astype(BF16)

    def make_queries(l, rows_in):
        flat = jnp.dot(rows_in, wq[l], preferred_element_type=F32)
        return head_norm(flat, query_gain[l : l + 1], HEAD_DIM ** (-0.5))

    def put_dup(keys, values, rows):
        for kv in range(kv_heads):
            cols = slice(kv * HEAD_DIM, (kv + 1) * HEAD_DIM)
            kdup[kv, rows, :] = jnp.concatenate([keys[:, cols]] * 2, axis=1)
            vdup[kv, rows, :128] = jnp.concatenate([values[:, cols]] * 2, axis=1)

    def halo_copy(l, seg):
        rows = seg_rows(seg)
        return send(
            pair_made.at[l, rows],
            halo.at[l, rows],
            hs_sem.at[l, seg],
            hr_sem.at[l, seg],
            {"sp": lax.rem(me_sp + 1, n_sp)},
        )

    def start_halo(l, which):
        @pl.when(me_sp < n_sp - 1)
        def _():
            for seg in which:
                halo_copy(l, seg).start()

    def finish_halo(l, seg):
        @pl.when(me_sp > 0)
        def _():
            halo_copy(l, seg).wait_recv()
            got = halo[l, seg_rows(seg), :]
            put_dup(got[:, :kv_width], got[:, kv_width:], seg_rows(seg))

        @pl.when(me_sp == 0)
        def _():
            none = jnp.zeros((SEG, kv_width), BF16)
            put_dup(none, none, seg_rows(seg))

    def end_halo_sends(l):
        @pl.when(me_sp < n_sp - 1)
        def _():
            for seg in range(segs):
                halo_copy(l, seg).wait_send()

    lane = lax.broadcasted_iota(jnp.int32, (SEG, 128), 1)
    low_half = lane < HEAD_DIM

    def attend(l, seg):
        rows = seg_rows(seg)
        window = pl.ds(pl.multiple_of(seg * SEG, SEG), SPAN)
        key_pos = lax.broadcasted_iota(jnp.int32, (1, SPAN), 1)
        inside = me_sp * row_count + (seg - LEFT) * SEG + key_pos >= 0
        shut = jnp.where(inside, 0.0, masked_score)
        for kv in range(kv_heads):
            stack = []
            for p in range(group // 2):
                lower = (kv * group + 2 * p) * HEAD_DIM
                tile = queries[rows, lower : lower + 128]
                none = jnp.zeros_like(tile)
                stack += [jnp.where(low_half, tile, none), jnp.where(low_half, none, tile)]
            stacked = jnp.concatenate(stack, axis=0)
            scores = lax.dot_general(
                stacked, kdup[kv, window, :], (((1,), (1,)), ((), ())), preferred_element_type=F32
            )
            base = kv * group * SEG
            scores = scores + bias[l, base : base + group * SEG, :SPAN] + shut
            peak = jnp.max(scores, axis=-1, keepdims=True)
            expon = jnp.exp(scores - peak).astype(BF16)
            summed = jnp.dot(expon, vdup[kv, window, :], preferred_element_type=F32)
            made = summed[:, :128] / summed[:, 128:]
            for p in range(group // 2):
                lower = (kv * group + 2 * p) * HEAD_DIM
                even = made[2 * p * SEG : (2 * p + 1) * SEG]
                odd = made[(2 * p + 1) * SEG : (2 * p + 2) * SEG]
                mixed[:, lower : lower + 128] = jnp.where(low_half, even, odd).astype(BF16)

    def project_out(l, lower, size):
        cols = pl.ds(pl.multiple_of(lower, 128), size)
        return jnp.dot(mixed[...], wo[l, :, cols], preferred_element_type=F32)

    def meet():
        at_edge = jnp.logical_or(me_sp == 0, me_sp == n_sp - 1)

        @pl.when(at_edge)
        def _():
            pl.semaphore_wait(barrier, n_x + min(n_sp - 1, 1))

        @pl.when(jnp.logical_not(at_edge))
        def _():
            pl.semaphore_wait(barrier, n_x + 2)

    for n, part in enumerate(parts):
        stream_loads[n].wait()
        if n == 0:
            gain_loads[0].wait()
        normed[part, :] = row_norm(cur0[part, :].astype(F32), attn_gain[0:1])
        if n == 0:
            for copy in gain_loads[1:]:
                copy.wait()
            weight_loads[0][0].wait()
            weight_loads[0][1].wait()
        keys, values = keys_values(0, normed[part, :])
        pair_made[0, part, :] = jnp.concatenate([keys, values], axis=1)
        if n == 0:
            meet()
        first_seg = (1 - n) * (segs // 2)
        start_halo(0, reversed(range(first_seg, first_seg + segs // 2)))
        put_dup(keys, values, pl.ds(row_count + (1 - n) * part_rows, part_rows))
    weight_loads[0][2].wait()
    queries[...] = make_queries(0, normed[...])
    build_bias(0)
    weight_loads[0][3].wait()

    def mine_at(i):
        return (half - 1 - i) * 2 + core

    def theirs_at(i):
        return (half - 1 - i) * 2 + 1 - core

    def partner_copy(i):
        return send(psend.at[i], precv.at[i], ps_sem.at[i], pr_sem.at[i], partner)

    sub = SEG // SUBS

    def chip_copy(i, j, k):
        rows = pl.ds(j * sub, sub)
        return send(
            xsend.at[i, rows],
            xrecv.at[k - 1, i, rows],
            xs_sem.at[k - 1, i, j],
            xr_sem.at[k - 1, i, j],
            peer(k),
        )

    def sub_rows(seg, j):
        return pl.ds(pl.multiple_of(seg * SEG + j * sub, sub), sub)

    def rows_copy(i, j, seg):
        rows = sub_rows(seg, j)
        return send(cur1.at[rows], cur1.at[rows], cs_sem.at[i, j], cr_sem.at[i, j], partner)

    out_step = min(width, 512)

    def first_out(i, carry):
        finish_halo(0, (half - 1 - i) * 2 + 1)
        finish_halo(0, (half - 1 - i) * 2)
        attend(0, theirs_at(i))
        for lower in range(0, width, out_step):
            psend[i, :, lower : lower + out_step] = project_out(0, lower, out_step).astype(BF16)
        partner_copy(i).start()
        attend(0, mine_at(i))
        for lower in range(0, width, out_step):
            own0[i, :, lower : lower + out_step] = project_out(0, lower, out_step)
        partner_copy(i).wait_recv()
        for j in range(SUBS):
            rows = slice(j * sub, (j + 1) * sub)
            both = own0[i, rows, :] + precv[i, rows, :].astype(F32)
            own0[i, rows, :] = both
            xsend[i, rows, :] = both.astype(BF16)
            for k in range(1, n_x):
                chip_copy(i, j, k).start()
        return carry

    lax.fori_loop(0, half, first_out, 0)
    build_bias(1)

    for l in range(1, LAYERS):
        for copy in weight_loads[l]:
            copy.wait()

    for i in range(half):
        mine = mine_at(i)
        theirs = theirs_at(i)
        for j in range(SUBS):
            total = own0[i, j * sub : (j + 1) * sub, :]
            for k in range(1, n_x):
                chip_copy(i, j, k).wait_recv()
                total = total + xrecv[k - 1, i, j * sub : (j + 1) * sub, :].astype(F32)
            rows = sub_rows(mine, j)
            summed = (cur0[rows, :].astype(F32) + total).astype(BF16)
            cur1[rows, :] = summed
            rows_copy(i, j, mine).start()
            normed[j * sub : (j + 1) * sub, :] = row_norm(summed.astype(F32), attn_gain[1:2])
        for j in range(SUBS):
            rows_copy(i, j, theirs).wait_recv()
            normed[SEG + j * sub : SEG + (j + 1) * sub, :] = row_norm(
                cur1[sub_rows(theirs, j), :].astype(F32), attn_gain[1:2]
            )
        rows_in = normed[0 : 2 * SEG, :]
        keys, values = keys_values(1, rows_in)
        made = jnp.concatenate([keys, values], axis=1)
        for n, seg in enumerate((mine, theirs)):
            part = slice(n * SEG, (n + 1) * SEG)
            pair_made[1, seg_rows(seg), :] = made[part]
        start_halo(1, (mine, theirs))
        for n, seg in enumerate((mine, theirs)):
            part = slice(n * SEG, (n + 1) * SEG)
            put_dup(keys[part], values[part], seg_rows(seg + segs))
        made_q = make_queries(1, rows_in)
        for n, seg in enumerate((mine, theirs)):
            queries[seg_rows(seg), :] = made_q[n * SEG : (n + 1) * SEG]

    def partner_copy1(s):
        return send(psend1.at[s], precv1.at[s], ps1_sem.at[s], pr1_sem.at[s], partner)

    def chip_copy1(s, k):
        return send(
            xsend1.at[k - 1, s],
            xrecv1.at[k - 1, s],
            xs1_sem.at[k - 1, s],
            xr1_sem.at[k - 1, s],
            peer(k),
        )

    def last_sends(s):
        partner_copy1(s).wait_recv()
        for k in range(n_x):
            both = own1[s, k] + precv1[s, k].astype(F32)
            if k == 0:
                own1[s, k] = both
            else:
                xsend1[k - 1, s] = both.astype(BF16)
                chip_copy1(s, k).start()

    def last_out(s, carry):
        finish_halo(1, segs - 1 - s)
        attend(1, segs - 1 - s)
        for k in range(n_x):
            lower = (chip_at(k) * 2 + 1 - core) * feat
            psend1[s, k] = project_out(1, lower, feat).astype(BF16)
        partner_copy1(s).start()
        for k in range(n_x):
            lower = (chip_at(k) * 2 + core) * feat
            own1[s, k] = project_out(1, lower, feat)

        @pl.when(s > 0)
        def _():
            last_sends(s - 1)

        return carry

    lax.fori_loop(0, segs, last_out, 0)
    last_sends(segs - 1)
    my_cols = pl.ds(pl.multiple_of(me_tp * feat, 128), feat)
    for s in range(segs):
        rows = slice((segs - 1 - s) * SEG, (segs - s) * SEG)
        total = own1[s, 0]
        for k in range(1, n_x):
            chip_copy1(s, k).wait_recv()
            total = total + xrecv1[k - 1, s].astype(F32)
        out[rows, :] = (cur1[rows, my_cols].astype(F32) + total).astype(BF16)

    for i in range(half):
        partner_copy(i).wait_send()
        for j in range(SUBS):
            rows_copy(i, j, mine_at(i)).wait_send()
            for k in range(1, n_x):
                chip_copy(i, j, k).wait_send()
    for s in range(segs):
        partner_copy1(s).wait_send()
        for k in range(1, n_x):
            chip_copy1(s, k).wait_send()
    for l in range(LAYERS):
        end_halo_sends(l)


def local(n_sp, n_tp, stream, attn_gain, w_query, w_key, w_value, w_out, query_gain, key_gain, rel_bias):
    row_count, width = stream.shape
    segs = row_count // SEG
    assert row_count == LEFT * SEG and n_tp % 2 == 0
    half = segs // 2
    n_x = n_tp // 2
    feat = width // n_tp
    q_width = w_query.shape[2]
    kv_width = w_key.shape[2]
    kv_heads = kv_width // HEAD_DIM
    heads = q_width // HEAD_DIM
    others = max(n_x - 1, 1)
    dma = pltpu.SemaphoreType.DMA
    anyw = pl.BlockSpec(memory_space=pltpu.HBM)
    vmem = pl.BlockSpec(memory_space=pltpu.VMEM)
    scratch = [
        pltpu.VMEM(attn_gain.shape, F32),
        pltpu.VMEM(query_gain.shape, F32),
        pltpu.VMEM(key_gain.shape, F32),
        pltpu.VMEM(rel_bias.shape, F32),
        pltpu.VMEM((row_count, width), BF16),
        pltpu.VMEM((row_count, width), BF16),
        pltpu.VMEM((row_count, width), BF16),
        pltpu.VMEM(w_query.shape, BF16),
        pltpu.VMEM(w_key.shape, BF16),
        pltpu.VMEM(w_value.shape, BF16),
        pltpu.VMEM(w_out.shape, BF16),
        pltpu.VMEM((row_count, q_width), BF16),
        pltpu.VMEM((LAYERS, row_count, 2 * kv_width), BF16),
        pltpu.VMEM((LAYERS, row_count, 2 * kv_width), BF16),
        pltpu.VMEM((kv_heads, 2 * row_count, 128), BF16),
        pltpu.VMEM((kv_heads, 2 * row_count, 256), BF16),
        pltpu.VMEM((LAYERS, heads * SEG, LINE), F32),
        pltpu.VMEM((SEG, q_width), BF16),
        pltpu.VMEM((half, SEG, width), BF16),
        pltpu.VMEM((half, SEG, width), BF16),
        pltpu.VMEM((half, SEG, width), F32),
        pltpu.VMEM((half, SEG, width), BF16),
        pltpu.VMEM((others, half, SEG, width), BF16),
        pltpu.VMEM((segs, n_x, SEG, feat), BF16),
        pltpu.VMEM((segs, n_x, SEG, feat), BF16),
        pltpu.VMEM((segs, n_x, SEG, feat), F32),
        pltpu.VMEM((others, segs, SEG, feat), BF16),
        pltpu.VMEM((others, segs, SEG, feat), BF16),
        dma((6 + 4 * LAYERS,)),
        dma((half,)), dma((half,)),
        dma((others, half, SUBS)), dma((others, half, SUBS)),
        dma((half, SUBS)), dma((half, SUBS)),
        dma((LAYERS, segs)), dma((LAYERS, segs)),
        dma((segs,)), dma((segs,)),
        dma((others, segs)), dma((others, segs)),
    ]
    return pl.pallas_call(
        functools.partial(body, n_sp, n_tp),
        out_shape=pltpu.VMEM((row_count, feat), BF16),
        in_specs=[anyw] * 9,
        out_specs=vmem,
        scratch_shapes=scratch,
        compiler_params=pltpu.CompilerParams(
            collective_id=0, has_side_effects=True, vmem_limit_bytes=60 * 1024 * 1024
        ),
    )(stream, attn_gain, w_query, w_key, w_value, w_out, query_gain, key_gain, rel_bias)


def solution(mesh):
    return jax.shard_map(
        functools.partial(local, mesh.shape["sp"], mesh.shape["tp"]),
        mesh=mesh,
        in_specs=(
            P("sp", None),
            P(),
            P(None, None, "tp"),
            P(None, None, "tp"),
            P(None, None, "tp"),
            P(None, "tp", None),
            P(),
            P(),
            P(None, "tp", None),
        ),
        out_specs=P("sp", "tp"),
        check_vma=False,
    )
```
